32 devices in a mesh: ep: 4 (over y, x), tp: 8 (over z, core).
Axes of the slice: x: 2, y: 2, z: 4, core: 2. Of those that a mesh axis runs over, the one named last changes fastest.
Arguments:
- tokens: bfloat16 [256, 2048], P('ep', 'tp'), may hold values from -6 to 6
- norm_gain: float32 [2048], replicated, may hold values from 0.5 to 1.5
- group_pick: int32 [256, 1], P('ep'), may hold values from 0 to 3; in each aligned block of 64 rows (0 to 63, 64 to 127, ...) at most 64 rows name the same one
- inner_pick: int32 [256, 2], P('ep'), may hold values from 0 to 3, all different within a row
- route_weight: float32 [256, 2], P('ep'), may hold values from 0.3 to 1
- w_gate: bfloat16 [16, 1024, 2048], P('ep', 'tp'), may hold values from -0.125 to 0.125
- w_up: bfloat16 [16, 1024, 2048], P('ep', 'tp'), may hold values from -0.125 to 0.125
- w_down: bfloat16 [16, 1024, 2048], P('ep', 'tp'), may hold values from -0.1875 to 0.1875
Outputs:
- mixed: bfloat16 [256, 2048], P('ep', 'tp')
The draws below stay inside these ranges and needn't reach their ends.
Inputs may be any that keep to these rules, and one draw needn't show every extreme that they name: `group_pick`: every entry is a group, 0 to 3; among the 64 tokens of any one index of ep no group is chosen more than 64 times, a bound that some block reaches. `inner_pick`: each row names 2 different experts of the chosen group, each 0 to 3.
All inputs are finite; a program needn't handle non-finite values.
Results may differ from the reference program's by a relative error of at most 0.002.
Values may be sent and summed in bfloat16 or wider, within the bound.
A program may use at most 64 MiB of HBM per device.

```python
import math
import jax
import jax.numpy as jnp
import numpy as np
from jax import lax

D = 2048
FF = 1024
EXP_GROUP = 4
TOP = 2
TOK_DEV = 64
GROUPS = 4
EXPERTS = 16
TOKENS = 256
CAP = 64


def levels(key, dims, pieces, low, largest):
    def one(dim, shards_of):
        heights = jax.random.uniform(jax.random.fold_in(jax.random.fold_in(key, 6), dim), (shards_of,), jnp.float32, low / len(pieces), largest / len(pieces))
        return jnp.repeat(jnp.exp(heights), dims[dim] // shards_of).reshape((-1,) + (1,) * (len(dims) - dim - 1))

    gain = one(*pieces[0])
    for cut in pieces[1:]:
        gain = gain * one(*cut)
    return gain


def choose_distinct(rng, rows, number_of, top, lift):
    sequence = jax.random.permutation(jax.random.fold_in(rng, 1), number_of)
    favour = sequence
    for power in range(3):
        favour = favour * favour // number_of
    favour = favour * lift // number_of
    chance = jax.random.randint(jax.random.fold_in(rng, 2), (rows, number_of), 0, 4096) + favour
    fixed_rows = jax.random.permutation(jax.random.fold_in(rng, 3), rows)[jnp.arange(number_of) % rows]
    chance = jnp.where(jnp.arange(rows)[:, None] == fixed_rows[None, :], 1 << 14, chance)
    merit = chance * number_of + jnp.arange(number_of)
    return lax.top_k(merit.astype(jnp.int32), top)[1].astype(jnp.int32)


def shared_out(rng, own, number, rows, count, top, most, slope):
    ranking = jax.random.permutation(rng, count)
    crowded, common = load_shares(count, rows * top, most, slope, True), load_shares(count, rows * top, most, slope, False)
    places = jnp.arange(count)

    def named(sizes, offset_by):
        used = int((sizes > 0).sum())
        fixed = max(1, used // 4)
        passed = fixed + (places - fixed + offset_by * (used - fixed)) % max(1, count - fixed)
        return jnp.zeros((count,), jnp.int32).at[ranking[jnp.where(places < fixed, places, passed)]].set(jnp.asarray(sizes, jnp.int32))

    sizes = jnp.where(number % 4 == 0, named(crowded, number // 4), named(common, number - number // 4 - 1))
    mixed = jax.random.permutation(jax.random.fold_in(own, 3), count)
    donor, taker = mixed[0:count // 2 * 2:2], mixed[1:count // 2 * 2:2]
    room = jnp.minimum(sizes[donor] - 1, most - sizes[taker]) // 2
    room = jnp.where((donor == ranking[0]) | (taker == ranking[0]) | (sizes[taker] == 0), 0, jnp.maximum(room, 0))
    passed = jax.random.randint(jax.random.fold_in(own, 4), (count // 2,), 0, 1 << 20) % (room + 1)
    sizes = sizes.at[donor].add(-passed).at[taker].add(passed)
    members = jnp.searchsorted(jnp.cumsum(sizes), jnp.arange(rows * top), side="right").astype(jnp.int32)
    table = members.reshape(top, rows).T
    table = table[jax.random.permutation(jax.random.fold_in(own, 1), rows)]
    offset_by = jax.random.randint(jax.random.fold_in(own, 2), (rows, 1), 0, top)
    return jnp.take_along_axis(table, (jnp.arange(top)[None, :] + offset_by) % top, axis=1)


def load_shares(amount, total, limit, skew, full):
    loads = [(1 << 20) // math.isqrt(rank ** skew) + 1 for rank in range(1, amount + 1)]
    largest = limit if full else min(limit, max(-(-total // amount), total * loads[0] // sum(loads)))
    least = 1 if total - largest >= amount - 1 else 0
    given, spare = [largest] + [least] * (amount - 1), total - largest - least * (amount - 1)
    while spare > 0:
        candidates = [i for i in range(1, amount) if given[i] < largest] or [i for i in range(1, amount) if given[i] < limit]
        pool, remaining = sum([loads[i] for i in candidates]), spare
        for i in candidates:
            addition = min(limit - given[i], max(1, remaining * loads[i] // pool), spare)
            given[i] = given[i] + addition
            spare = spare - addition
    return np.array(given)


def bell_draw(own_key, extent, scale, bound, cuts=(), kind=jnp.bfloat16):
    result = jax.random.normal(own_key, extent, jnp.float32) * scale
    if len(cuts) > 0:
        result = levels(own_key, extent, cuts, -0.22, 0.18) * result
    return jnp.clip(result, min=-bound, max=bound).astype(kind)


def setup_inputs(seed: int = 0) -> dict:
    splits = jax.random.split(jax.random.key(seed), 9)
    tokens = bell_draw(splits[0], (TOKENS, D), 1.0, 6.0, ((0, 4), (1, 8)))
    norm_gain = jnp.clip(1.0 + 0.1 * jax.random.normal(splits[1], (D,), jnp.float32), 0.5, 1.5)
    group_pick_keys = jax.random.split(jax.random.fold_in(splits[2], 1), TOKENS // TOK_DEV)
    group_pick_turns = jax.random.permutation(jax.random.fold_in(splits[2], 3), TOKENS // TOK_DEV)
    group_pick = jax.vmap(lambda own, number: shared_out(jax.random.fold_in(splits[2], 2), own, number, TOK_DEV, GROUPS, 1, CAP, 2))(group_pick_keys, group_pick_turns).reshape((TOKENS, 1))
    inner_pick = choose_distinct(splits[3], TOKENS, EXP_GROUP, TOP, 0)
    route_weight = jnp.clip(0.3 + 0.7 * jax.random.uniform(splits[4], (TOKENS, TOP), jnp.float32) ** levels(splits[4], (TOKENS, TOP), ((0, 4),), -0.2, 0.2), 0.3, 1.0)
    w_gate = bell_draw(splits[5], (EXPERTS, FF, D), D ** -0.5, 0.125, ((0, 4), (1, 8)))
    w_up = bell_draw(splits[6], (EXPERTS, FF, D), D ** -0.5, 0.125, ((0, 4), (1, 8)))
    w_down = bell_draw(splits[7], (EXPERTS, FF, D), FF ** -0.5, 0.1875, ((0, 4), (1, 8)))
    return dict(tokens=tokens, norm_gain=norm_gain, group_pick=group_pick, inner_pick=inner_pick, route_weight=route_weight, w_gate=w_gate, w_up=w_up, w_down=w_down)


epsilon = 1e-06

def reference(tokens, norm_gain, group_pick, inner_pick, route_weight, w_gate, w_up, w_down):
    widened = tokens.astype(jnp.float32)
    scaled = lax.rsqrt(lax.optimization_barrier(jnp.mean(widened * widened, axis=-1, keepdims=True)) + epsilon)
    normed = (widened * scaled * norm_gain).astype(jnp.bfloat16)
    chosen = (group_pick * EXP_GROUP + inner_pick).astype(jnp.int32)

    def one_token(packed):
        token_row, token_picks, token_weights = packed
        running = jnp.zeros((D,), jnp.float32)
        for ordinal in range(TOP):
            expert = token_picks[ordinal]
            gate_proj = jnp.dot(w_gate[expert], token_row, preferred_element_type=jnp.float32)
            up_proj = jnp.dot(w_up[expert], token_row, preferred_element_type=jnp.float32)
            hidden = (jax.nn.silu(gate_proj) * up_proj).astype(jnp.bfloat16)
            product = jnp.dot(hidden, w_down[expert], preferred_element_type=jnp.float32)
            running = running + token_weights[ordinal] * product
        return running
    mixed_rows = lax.map(one_token, (normed, chosen, route_weight))
    return mixed_rows.astype(jnp.bfloat16)
```

```python
import functools

import jax
import jax.numpy as jnp
from jax import lax
from jax.experimental import pallas as pl
from jax.experimental.pallas import tpu as pltpu
from jax.sharding import PartitionSpec as P

epsilon = 1e-06
MESH = pl.DeviceIdType.MESH


def fused_kernel(
    nz,
    tokens,
    gain,
    group_pick,
    inner_pick,
    route_weight,
    wg_hbm,
    wu_hbm,
    wd_hbm,
    out,
    wg,
    wu,
    wd,
    rows,
    gates,
    normed,
    hcat,
    to_core,
    from_core,
    part_a,
    part_b,
    in_a1,
    in_b1,
    in_a2,
    in_b2,
    fin,
    in_z,
    w_sem,
    row_send,
    row_recv,
    gate_send,
    gate_recv,
    core_send,
    core_recv,
    xy_send,
    xy_recv,
    z_send,
    z_recv,
):
    ep, tp = lax.axis_index("ep"), lax.axis_index("tp")
    z, core = tp // 2, tp % 2
    twin = (ep, z * 2 + (1 - core))
    peer = [None, (ep ^ 1, tp), (ep ^ 2, tp), (ep ^ 3, tp)]
    tok, share = tokens.shape
    inner = wd_hbm.shape[0]
    width = wd_hbm.shape[1]
    half = share // 2

    def at_z(dz):
        return lax.rem(z + dz, nz)

    loads = [
        pltpu.make_async_copy(src, dst, w_sem.at[i])
        for i, (src, dst) in enumerate(((wg_hbm, wg), (wu_hbm, wu), (wd_hbm, wd)))
    ]
    for load in loads:
        load.start()

    barrier = pltpu.get_barrier_semaphore()
    greeted = [twin] + peer[1:] + [(ep, at_z(dz) * 2 + core) for dz in range(1, nz)]
    for device in greeted:
        pl.semaphore_signal(barrier, inc=1, device_id=device, device_id_type=MESH)

    lane = lax.broadcasted_iota(jnp.int32, (tok, 128), 1)
    relative = (group_pick[...] ^ ep) * inner
    table = jnp.zeros((tok, 128), jnp.float32)
    for k in range(inner_pick.shape[1]):
        key = relative + inner_pick[:, k : k + 1]
        table = table + jnp.where(lane == key, route_weight[:, k : k + 1], 0.0)
    table = jnp.concatenate([table, jnp.zeros((128 - tok, 128), jnp.float32)], axis=0)
    gates[0] = jnp.transpose(table)[: gates.shape[1], :]
    rows[0, tp] = tokens[...]

    pl.semaphore_wait(barrier, len(greeted))

    sent = []

    def send(src, dst, send_sem, recv_sem, device):
        copy = pltpu.make_async_remote_copy(
            src_ref=src,
            dst_ref=dst,
            send_sem=send_sem,
            recv_sem=recv_sem,
            device_id=device,
            device_id_type=MESH,
        )
        copy.start()
        sent.append(copy)

    def arrived(dst, recv_sem):
        pltpu.make_async_remote_copy(
            src_ref=dst,
            dst_ref=dst,
            send_sem=recv_sem,
            recv_sem=recv_sem,
            device_id=twin,
            device_id_type=MESH,
        ).wait_recv()

    counter = [0]

    def send_row(src, r, t, device):
        i = counter[0]
        counter[0] += 1
        send(src, rows.at[r, t], row_send.at[i], row_recv.at[r, t], device)

    def row_arrived(r, t):
        arrived(rows.at[r, t], row_recv.at[r, t])

    for dz in range(1, nz):
        send_row(tokens, 0, tp, (ep, at_z(dz) * 2 + core))
    send_row(tokens, 1, tp, peer[1])
    send_row(tokens, 2, tp, peer[2])
    send_row(tokens, 0, tp, twin)
    for r in range(1, 4):
        send(gates.at[0], gates.at[r], gate_send.at[r], gate_recv.at[r], peer[r])
    order = sorted(range(nz), key=lambda dz: min(dz, nz - dz))
    for dz in order[1:]:
        t = at_z(dz) * 2 + core
        row_arrived(0, t)
        send_row(rows.at[0, t], 1, t, peer[1])
        send_row(rows.at[0, t], 2, t, peer[2])
        send_row(rows.at[0, t], 0, t, twin)
    for i, dz in enumerate(order):
        t = at_z(dz) * 2 + core
        row_arrived(1, t)
        if i % 2 == 0:
            send_row(rows.at[1, t], 3, t, peer[2])
        send_row(rows.at[1, t], 1, t, twin)
        row_arrived(2, t)
        if i % 2 == 1:
            send_row(rows.at[2, t], 3, t, peer[1])
        send_row(rows.at[2, t], 2, t, twin)
    for dz in order:
        t = at_z(dz) * 2 + core
        row_arrived(3, t)
        send_row(rows.at[3, t], 3, t, twin)

    columns = []
    for r in range(4):
        if r > 0:
            arrived(gates.at[r], gate_recv.at[r])
        for dz in range(nz):
            row_arrived(r, at_z(dz) * 2 + (1 - core))
        total = jnp.zeros((tok, 1), jnp.float32)
        for t in range(2 * nz):
            piece = rows[r, t].astype(jnp.float32)
            total = total + jnp.sum(piece * piece, axis=1, keepdims=True)
        scaled = lax.rsqrt(total / (2 * nz * share) + epsilon)
        for t in range(2 * nz):
            piece = rows[r, t].astype(jnp.float32)
            span = slice(t * share, (t + 1) * share)
            normed[r * tok : (r + 1) * tok, span] = (piece * scaled * gain[:, span]).astype(jnp.bfloat16)
        turned = jnp.transpose(gates[r])[:tok]
        columns.append([turned[:, r * inner + e : r * inner + e + 1] for e in range(inner)])

    loads[0].wait()
    loads[1].wait()
    count = 4 * tok
    contract = (((1,), (1,)), ((), ()))
    for e in range(0, inner, 2):
        pair = wg[e : e + 2].reshape(2 * width, -1)
        gate_proj = lax.dot_general(normed[...], pair, contract, preferred_element_type=jnp.float32)
        pair = wu[e : e + 2].reshape(2 * width, -1)
        up_proj = lax.dot_general(normed[...], pair, contract, preferred_element_type=jnp.float32)
        hidden = gate_proj / (1.0 + jnp.exp(-gate_proj)) * up_proj
        hidden = hidden.astype(jnp.bfloat16).astype(jnp.float32)
        for j in range(2):
            weight = jnp.concatenate([columns[r][e + j] for r in range(4)], axis=0)
            weighted = hidden[:, j * width : (j + 1) * width] * weight
            high = weighted.astype(jnp.bfloat16)
            low = (weighted - high.astype(jnp.float32)).astype(jnp.bfloat16)
            span = slice((e + j) * width, (e + j + 1) * width)
            hcat[:count, span] = high
            hcat[count:, span] = low

    loads[2].wait()

    def down(t):
        cols = pl.ds(pl.multiple_of(t * share, share), share)
        both = jnp.dot(
            hcat[...],
            wd[:, :, cols].reshape(inner * width, share),
            preferred_element_type=jnp.float32,
        )
        return both[:count] + both[count:]

    offsets = sorted(range(1, nz), key=lambda dz: -min(dz, nz - dz)) + [0]
    for k, dz in enumerate(offsets):
        to_core[k] = down(at_z(dz) * 2 + (1 - core))
        send(to_core.at[k], from_core.at[k], core_send.at[k], core_recv.at[k], twin)
        mine = down(at_z(dz) * 2 + core)
        arrived(from_core.at[k], core_recv.at[k])
        for slot in range(4):
            ra = (0, 2, 1, 3)[slot]
            part_a[k, slot] = (
                mine[ra * tok : (ra + 1) * tok, :half] + from_core[k, ra * tok : (ra + 1) * tok, :half]
            )
            part_b[k, slot] = (
                mine[slot * tok : (slot + 1) * tok, half:] + from_core[k, slot * tok : (slot + 1) * tok, half:]
            )
        send(part_a.at[k, pl.ds(2, 2)], in_a1.at[k], xy_send.at[k, 0], xy_recv.at[k, 0], peer[1])
        send(part_b.at[k, pl.ds(2, 2)], in_b1.at[k], xy_send.at[k, 1], xy_recv.at[k, 1], peer[2])

    def second(k):
        arrived(in_a1.at[k], xy_recv.at[k, 0])
        part_a[k, 1] += in_a1[k, 1]
        send(part_a.at[k, 1], in_a2.at[k], xy_send.at[k, 2], xy_recv.at[k, 2], peer[2])
        arrived(in_b1.at[k], xy_recv.at[k, 1])
        part_b[k, 1] += in_b1[k, 1]
        send(part_b.at[k, 1], in_b2.at[k], xy_send.at[k, 3], xy_recv.at[k, 3], peer[1])

    def last(k):
        arrived(in_a2.at[k], xy_recv.at[k, 2])
        fin[k, :, :half] = part_a[k, 0] + in_a1[k, 0] + in_a2[k]
        arrived(in_b2.at[k], xy_recv.at[k, 3])
        fin[k, :, half:] = part_b[k, 0] + in_b1[k, 0] + in_b2[k]
        if offsets[k] != 0:
            device = (ep, at_z(offsets[k]) * 2 + core)
            send(fin.at[k], in_z.at[k], z_send.at[k], z_recv.at[k], device)

    for k in range(nz):
        second(k)
        if k > 0:
            last(k - 1)
    last(nz - 1)
    total = fin[nz - 1]
    for k in range(nz - 1):
        arrived(in_z.at[k], z_recv.at[k])
        total = total + in_z[k]
    out[...] = total.astype(out.dtype)
    for copy in sent:
        copy.wait_send()


def fused(tokens, norm_gain, group_pick, inner_pick, route_weight, w_gate, w_up, w_down):
    tp_size = lax.axis_size("tp")
    nz = tp_size // 2
    tok, share = tokens.shape
    inner, width, features = w_gate.shape
    half = share // 2
    count = 4 * tok
    gate_rows = -(-4 * inner // 8) * 8
    f32, bf16 = jnp.float32, jnp.bfloat16
    vmem = pl.BlockSpec(memory_space=pltpu.VMEM)
    hbm = pl.BlockSpec(memory_space=pl.ANY)
    dma = pltpu.SemaphoreType.DMA
    sends = (nz - 1) + 3 + 3 * (nz - 1) + 3 * nz + nz
    return pl.pallas_call(
        functools.partial(fused_kernel, nz),
        out_shape=jax.ShapeDtypeStruct((tok, share), bf16),
        in_specs=[vmem] * 5 + [hbm] * 3,
        out_specs=vmem,
        scratch_shapes=[
            pltpu.VMEM((inner, width, features), bf16),
            pltpu.VMEM((inner, width, features), bf16),
            pltpu.VMEM((inner, width, features), bf16),
            pltpu.VMEM((4, tp_size, tok, share), bf16),
            pltpu.VMEM((4, gate_rows, 128), f32),
            pltpu.VMEM((count, features), bf16),
            pltpu.VMEM((2 * count, inner * width), bf16),
            pltpu.VMEM((nz, count, share), f32),
            pltpu.VMEM((nz, count, share), f32),
            pltpu.VMEM((nz, 4, tok, half), f32),
            pltpu.VMEM((nz, 4, tok, half), f32),
            pltpu.VMEM((nz, 2, tok, half), f32),
            pltpu.VMEM((nz, 2, tok, half), f32),
            pltpu.VMEM((nz, tok, half), f32),
            pltpu.VMEM((nz, tok, half), f32),
            pltpu.VMEM((nz, tok, share), f32),
            pltpu.VMEM((nz, tok, share), f32),
            dma((3,)),
            dma((sends,)),
            dma((4, tp_size)),
            dma((4,)),
            dma((4,)),
            dma((nz,)),
            dma((nz,)),
            dma((nz, 4)),
            dma((nz, 4)),
            dma((nz,)),
            dma((nz,)),
        ],
        compiler_params=pltpu.CompilerParams(
            collective_id=0, has_side_effects=True, vmem_limit_bytes=48 * 1024 * 1024
        ),
    )(tokens, norm_gain.reshape(1, -1), group_pick, inner_pick, route_weight, w_gate, w_up, w_down)


def scattered(portion, rows, axis):
    count = rows * lax.axis_size(axis)
    return lax.psum_scatter(portion(jnp.int32(0), count), axis, scatter_dimension=0, tiled=True)


def rms_normed(rows, norm_gain):
    widened = rows.astype(jnp.float32)
    scaled = lax.rsqrt(jnp.mean(widened * widened, axis=-1, keepdims=True) + epsilon)
    return (widened * scaled * norm_gain).astype(jnp.bfloat16)


def per_device(tokens, norm_gain, group_pick, inner_pick, route_weight, w_gate, w_up, w_down):
    ep_size = lax.axis_size("ep")
    tok_rows = tokens.shape[0]
    feature_share = tokens.shape[1]
    inner_count = w_gate.shape[0]
    capacity = min(tok_rows, 4 * tok_rows // ep_size + 2)
    slot_count = ep_size * capacity
    groups = group_pick[:, 0]
    member = (groups[:, None] == jnp.arange(ep_size, dtype=jnp.int32)[None, :]).astype(jnp.int32)
    earlier = jnp.sum((jnp.cumsum(member, axis=0) - member) * member, axis=1)
    position = (groups * capacity + earlier).astype(jnp.int32)
    placing = position[None, :] == jnp.arange(slot_count, dtype=jnp.int32)[:, None]
    local_gates = jnp.sum(
        jax.nn.one_hot(inner_pick, inner_count, dtype=jnp.float32) * route_weight[:, :, None],
        axis=1,
    )
    packed_rows = jnp.dot(
        placing.astype(jnp.bfloat16), tokens, preferred_element_type=jnp.float32
    ).astype(jnp.bfloat16)
    packed_gates = jnp.dot(
        placing.astype(jnp.float32), local_gates, precision=lax.Precision.HIGHEST
    )
    packed_rows = packed_rows.reshape(ep_size, capacity, feature_share)
    packed_gates = packed_gates.reshape(ep_size, capacity, inner_count)
    arrived_rows = lax.all_to_all(packed_rows, "ep", split_axis=0, concat_axis=0, tiled=True)
    arrived_gates = lax.all_to_all(packed_gates, "ep", split_axis=0, concat_axis=0, tiled=True)
    full_rows = lax.all_gather(arrived_rows, "tp", axis=2, tiled=True).reshape(slot_count, -1)
    normed = rms_normed(full_rows, norm_gain)
    gate_proj = jnp.einsum("sd,efd->esf", normed, w_gate, preferred_element_type=jnp.float32)
    up_proj = jnp.einsum("sd,efd->esf", normed, w_up, preferred_element_type=jnp.float32)
    hidden = (jax.nn.silu(gate_proj) * up_proj).astype(jnp.bfloat16)
    slot_gates = jnp.transpose(arrived_gates.reshape(slot_count, inner_count))

    def weighted_sum(down_part):
        products = jnp.einsum("esf,efd->esd", hidden, down_part, preferred_element_type=jnp.float32)
        return jnp.sum(slot_gates[:, :, None] * products, axis=0)

    def column_term(first_row, row_count):
        down_part = lax.dynamic_slice_in_dim(w_down, first_row, row_count, 2)
        return jnp.transpose(weighted_sum(down_part))

    own_share = scattered(column_term, feature_share, "tp")
    partial_rows = jnp.transpose(own_share).reshape(ep_size, capacity, feature_share)
    returned = (
        lax.all_to_all(
            partial_rows.astype(jnp.bfloat16), "ep", split_axis=0, concat_axis=0, tiled=True
        )
        .astype(partial_rows.dtype)
        .reshape(slot_count, feature_share)
    )
    mixed_rows = jnp.take(returned, position, axis=0)
    return mixed_rows.astype(jnp.bfloat16)


def solution(mesh):
    square = mesh.shape["ep"] == 4 and mesh.shape["tp"] % 2 == 0
    return jax.shard_map(
        fused if square else per_device,
        mesh=mesh,
        in_specs=(
            P("ep", "tp"),
            P(),
            P("ep", None),
            P("ep", None),
            P("ep", None),
            P("ep", "tp", None),
            P("ep", "tp", None),
            P("ep", "tp", None),
        ),
        out_specs=P("ep", "tp"),
        check_vma=False,
    )
```

```python
import functools

import jax
import jax.numpy as jnp
from jax import lax
from jax.experimental import pallas as pl
from jax.experimental.pallas import tpu as pltpu
from jax.sharding import PartitionSpec as P

epsilon = 1e-06
MESH = pl.DeviceIdType.MESH


def fused_kernel(
    nz,
    tokens_hbm,
    gain_hbm,
    group_hbm,
    inner_hbm,
    route_hbm,
    wg_hbm,
    wu_hbm,
    wd_hbm,
    out,
    tokens,
    gain,
    group_pick,
    inner_pick,
    route_weight,
    wg,
    wu,
    wd,
    rows,
    gates,
    normed,
    hcat,
    to_core,
    from_core,
    part_a,
    part_b,
    in_a1,
    in_b1,
    in_a2,
    in_b2,
    fin,
    in_z,
    w_sem,
    row_send,
    row_recv,
    gate_send,
    gate_recv,
    core_send,
    core_recv,
    xy_send,
    xy_recv,
    z_send,
    z_recv,
):
    ep, tp = lax.axis_index("ep"), lax.axis_index("tp")
    z, core = tp // 2, tp % 2
    twin = (ep, z * 2 + (1 - core))
    peer = [None, (ep ^ 1, tp), (ep ^ 2, tp), (ep ^ 3, tp)]
    tok, share = tokens.shape
    inner = wd_hbm.shape[0]
    width = wd_hbm.shape[1]
    half = share // 2

    def at_z(dz):
        return lax.rem(z + dz, nz)

    loads = [
        pltpu.make_async_copy(src, dst, w_sem.at[i])
        for i, (src, dst) in enumerate(
            (
                (tokens_hbm, tokens),
                (group_hbm, group_pick),
                (inner_hbm, inner_pick),
                (route_hbm, route_weight),
                (gain_hbm, gain),
                (wg_hbm, wg),
                (wu_hbm, wu),
                (wd_hbm, wd),
            )
        )
    ]
    for load in loads:
        load.start()

    barrier = pltpu.get_barrier_semaphore()
    greeted = [twin] + peer[1:] + [(ep, at_z(dz) * 2 + core) for dz in range(1, nz)]
    for device in greeted:
        pl.semaphore_signal(barrier, inc=1, device_id=device, device_id_type=MESH)

    for load in loads[:4]:
        load.wait()
    gate_rows = gates.shape[1]
    row = lax.broadcasted_iota(jnp.int32, (gate_rows, tok), 0)
    relative = (group_pick[...] ^ ep) * inner
    table = jnp.zeros((gate_rows, tok), jnp.float32)
    for k in range(inner_pick.shape[0]):
        key = relative + inner_pick[k : k + 1, :]
        table = table + jnp.where(row == key, route_weight[k : k + 1, :], 0.0)
    gates[0] = jnp.concatenate([table, jnp.zeros((gate_rows, 128 - tok), jnp.float32)], axis=1)
    rows[0, tp] = tokens[...]

    pl.semaphore_wait(barrier, len(greeted))

    sent = []

    def send(src, dst, send_sem, recv_sem, device):
        copy = pltpu.make_async_remote_copy(
            src_ref=src,
            dst_ref=dst,
            send_sem=send_sem,
            recv_sem=recv_sem,
            device_id=device,
            device_id_type=MESH,
        )
        copy.start()
        sent.append(copy)

    def arrived(dst, recv_sem):
        pltpu.make_async_remote_copy(
            src_ref=dst,
            dst_ref=dst,
            send_sem=recv_sem,
            recv_sem=recv_sem,
            device_id=twin,
            device_id_type=MESH,
        ).wait_recv()

    counter = [0]

    def send_row(src, r, t, device):
        i = counter[0]
        counter[0] += 1
        send(src, rows.at[r, t], row_send.at[i], row_recv.at[r, t], device)

    def row_arrived(r, t):
        arrived(rows.at[r, t], row_recv.at[r, t])

    for dz in range(1, nz):
        send_row(tokens, 0, tp, (ep, at_z(dz) * 2 + core))
    send_row(tokens, 1, tp, peer[1])
    send_row(tokens, 2, tp, peer[2])
    send_row(tokens, 0, tp, twin)
    for r in range(1, 4):
        send(gates.at[0], gates.at[r], gate_send.at[r], gate_recv.at[r], peer[r])
    order = sorted(range(nz), key=lambda dz: min(dz, nz - dz))
    for dz in order[1:]:
        t = at_z(dz) * 2 + core
        row_arrived(0, t)
        send_row(rows.at[0, t], 1, t, peer[1])
        send_row(rows.at[0, t], 2, t, peer[2])
        send_row(rows.at[0, t], 0, t, twin)

    columns = []

    def norm(r):
        if r > 0:
            arrived(gates.at[r], gate_recv.at[r])
        for dz in range(nz):
            row_arrived(r, at_z(dz) * 2 + (1 - core))
        total = jnp.zeros((tok, 1), jnp.float32)
        for t in range(2 * nz):
            piece = rows[r, t].astype(jnp.float32)
            total = total + jnp.sum(piece * piece, axis=1, keepdims=True)
        scaled = lax.rsqrt(total / (2 * nz * share) + epsilon)
        for t in range(2 * nz):
            piece = rows[r, t].astype(jnp.float32)
            span = slice(t * share, (t + 1) * share)
            normed[r * tok : (r + 1) * tok, span] = (piece * scaled * gain[:, span]).astype(jnp.bfloat16)
        turned = jnp.transpose(gates[r])[:tok]
        columns.append([turned[:, r * inner + e : r * inner + e + 1] for e in range(inner)])

    loads[4].wait()
    norm(0)
    for i, dz in enumerate(order):
        t = at_z(dz) * 2 + core
        row_arrived(1, t)
        if i % 2 == 0:
            send_row(rows.at[1, t], 3, t, peer[2])
        send_row(rows.at[1, t], 1, t, twin)
        row_arrived(2, t)
        if i % 2 == 1:
            send_row(rows.at[2, t], 3, t, peer[1])
        send_row(rows.at[2, t], 2, t, twin)
    norm(1)
    norm(2)
    for dz in order:
        t = at_z(dz) * 2 + core
        row_arrived(3, t)
        send_row(rows.at[3, t], 3, t, twin)
    norm(3)

    loads[5].wait()
    loads[6].wait()
    count = 4 * tok
    contract = (((1,), (1,)), ((), ()))
    for e in range(0, inner, 2):
        pair = wg[e : e + 2].reshape(2 * width, -1)
        gate_proj = lax.dot_general(normed[...], pair, contract, preferred_element_type=jnp.float32)
        pair = wu[e : e + 2].reshape(2 * width, -1)
        up_proj = lax.dot_general(normed[...], pair, contract, preferred_element_type=jnp.float32)
        hidden = gate_proj / (1.0 + jnp.exp(-gate_proj)) * up_proj
        hidden = hidden.astype(jnp.bfloat16).astype(jnp.float32)
        for j in range(2):
            weight = jnp.concatenate([columns[r][e + j] for r in range(4)], axis=0)
            weighted = hidden[:, j * width : (j + 1) * width] * weight
            high = weighted.astype(jnp.bfloat16)
            low = (weighted - high.astype(jnp.float32)).astype(jnp.bfloat16)
            span = slice((e + j) * width, (e + j + 1) * width)
            hcat[:count, span] = high
            hcat[count:, span] = low

    loads[7].wait()

    def down(t):
        cols = pl.ds(pl.multiple_of(t * share, share), share)
        both = jnp.dot(
            hcat[...],
            wd[:, :, cols].reshape(inner * width, share),
            preferred_element_type=jnp.float32,
        )
        return both[:count] + both[count:]

    offsets = sorted(range(1, nz), key=lambda dz: -min(dz, nz - dz)) + [0]
    for k, dz in enumerate(offsets):
        to_core[k] = down(at_z(dz) * 2 + (1 - core))
        send(to_core.at[k], from_core.at[k], core_send.at[k], core_recv.at[k], twin)
        mine = down(at_z(dz) * 2 + core)
        arrived(from_core.at[k], core_recv.at[k])
        for slot in range(4):
            ra = (0, 2, 1, 3)[slot]
            part_a[k, slot] = (
                mine[ra * tok : (ra + 1) * tok, :half] + from_core[k, ra * tok : (ra + 1) * tok, :half]
            )
            part_b[k, slot] = (
                mine[slot * tok : (slot + 1) * tok, half:] + from_core[k, slot * tok : (slot + 1) * tok, half:]
            )
        send(part_a.at[k, pl.ds(2, 2)], in_a1.at[k], xy_send.at[k, 0], xy_recv.at[k, 0], peer[1])
        send(part_b.at[k, pl.ds(2, 2)], in_b1.at[k], xy_send.at[k, 1], xy_recv.at[k, 1], peer[2])

    def second(k):
        arrived(in_a1.at[k], xy_recv.at[k, 0])
        part_a[k, 1] += in_a1[k, 1]
        send(part_a.at[k, 1], in_a2.at[k], xy_send.at[k, 2], xy_recv.at[k, 2], peer[2])
        arrived(in_b1.at[k], xy_recv.at[k, 1])
        part_b[k, 1] += in_b1[k, 1]
        send(part_b.at[k, 1], in_b2.at[k], xy_send.at[k, 3], xy_recv.at[k, 3], peer[1])

    def last(k):
        arrived(in_a2.at[k], xy_recv.at[k, 2])
        fin[k, :, :half] = part_a[k, 0] + in_a1[k, 0] + in_a2[k]
        arrived(in_b2.at[k], xy_recv.at[k, 3])
        fin[k, :, half:] = part_b[k, 0] + in_b1[k, 0] + in_b2[k]
        if offsets[k] != 0:
            device = (ep, at_z(offsets[k]) * 2 + core)
            send(fin.at[k], in_z.at[k], z_send.at[k], z_recv.at[k], device)

    for k in range(nz):
        second(k)
        if k > 0:
            last(k - 1)
    last(nz - 1)
    total = fin[nz - 1]
    for k in range(nz - 1):
        arrived(in_z.at[k], z_recv.at[k])
        total = total + in_z[k]
    out[...] = total.astype(out.dtype)
    for copy in sent:
        copy.wait_send()


def fused(tokens, norm_gain, group_pick, inner_pick, route_weight, w_gate, w_up, w_down):
    tp_size = lax.axis_size("tp")
    nz = tp_size // 2
    tok, share = tokens.shape
    inner, width, features = w_gate.shape
    half = share // 2
    top = inner_pick.shape[1]
    count = 4 * tok
    gate_rows = -(-4 * inner // 8) * 8
    f32, bf16 = jnp.float32, jnp.bfloat16
    vmem = pl.BlockSpec(memory_space=pltpu.VMEM)
    hbm = pl.BlockSpec(memory_space=pl.ANY)
    dma = pltpu.SemaphoreType.DMA
    sends = (nz - 1) + 3 + 3 * (nz - 1) + 3 * nz + nz
    return pl.pallas_call(
        functools.partial(fused_kernel, nz),
        out_shape=jax.ShapeDtypeStruct((tok, share), bf16),
        in_specs=[hbm] * 8,
        out_specs=vmem,
        scratch_shapes=[
            pltpu.VMEM((tok, share), bf16),
            pltpu.VMEM((1, features), f32),
            pltpu.VMEM((1, tok), jnp.int32),
            pltpu.VMEM((top, tok), jnp.int32),
            pltpu.VMEM((top, tok), f32),
            pltpu.VMEM((inner, width, features), bf16),
            pltpu.VMEM((inner, width, features), bf16),
            pltpu.VMEM((inner, width, features), bf16),
            pltpu.VMEM((4, tp_size, tok, share), bf16),
            pltpu.VMEM((4, gate_rows, 128), f32),
            pltpu.VMEM((count, features), bf16),
            pltpu.VMEM((2 * count, inner * width), bf16),
            pltpu.VMEM((nz, count, share), f32),
            pltpu.VMEM((nz, count, share), f32),
            pltpu.VMEM((nz, 4, tok, half), f32),
            pltpu.VMEM((nz, 4, tok, half), f32),
            pltpu.VMEM((nz, 2, tok, half), f32),
            pltpu.VMEM((nz, 2, tok, half), f32),
            pltpu.VMEM((nz, tok, half), f32),
            pltpu.VMEM((nz, tok, half), f32),
            pltpu.VMEM((nz, tok, share), f32),
            pltpu.VMEM((nz, tok, share), f32),
            dma((8,)),
            dma((sends,)),
            dma((4, tp_size)),
            dma((4,)),
            dma((4,)),
            dma((nz,)),
            dma((nz,)),
            dma((nz, 4)),
            dma((nz, 4)),
            dma((nz,)),
            dma((nz,)),
        ],
        compiler_params=pltpu.CompilerParams(
            collective_id=0, has_side_effects=True, vmem_limit_bytes=67043328
        ),
    )(
        tokens,
        norm_gain.reshape(1, -1),
        group_pick.T,
        inner_pick.T,
        route_weight.T,
        w_gate,
        w_up,
        w_down,
    )


def scattered(portion, rows, axis):
    count = rows * lax.axis_size(axis)
    return lax.psum_scatter(portion(jnp.int32(0), count), axis, scatter_dimension=0, tiled=True)


def rms_normed(rows, norm_gain):
    widened = rows.astype(jnp.float32)
    scaled = lax.rsqrt(jnp.mean(widened * widened, axis=-1, keepdims=True) + epsilon)
    return (widened * scaled * norm_gain).astype(jnp.bfloat16)


def per_device(tokens, norm_gain, group_pick, inner_pick, route_weight, w_gate, w_up, w_down):
    ep_size = lax.axis_size("ep")
    tok_rows = tokens.shape[0]
    feature_share = tokens.shape[1]
    inner_count = w_gate.shape[0]
    capacity = min(tok_rows, 4 * tok_rows // ep_size + 2)
    slot_count = ep_size * capacity
    groups = group_pick[:, 0]
    member = (groups[:, None] == jnp.arange(ep_size, dtype=jnp.int32)[None, :]).astype(jnp.int32)
    earlier = jnp.sum((jnp.cumsum(member, axis=0) - member) * member, axis=1)
    position = (groups * capacity + earlier).astype(jnp.int32)
    placing = position[None, :] == jnp.arange(slot_count, dtype=jnp.int32)[:, None]
    local_gates = jnp.sum(
        jax.nn.one_hot(inner_pick, inner_count, dtype=jnp.float32) * route_weight[:, :, None],
        axis=1,
    )
    packed_rows = jnp.dot(
        placing.astype(jnp.bfloat16), tokens, preferred_element_type=jnp.float32
    ).astype(jnp.bfloat16)
    packed_gates = jnp.dot(
        placing.astype(jnp.float32), local_gates, precision=lax.Precision.HIGHEST
    )
    packed_rows = packed_rows.reshape(ep_size, capacity, feature_share)
    packed_gates = packed_gates.reshape(ep_size, capacity, inner_count)
    arrived_rows = lax.all_to_all(packed_rows, "ep", split_axis=0, concat_axis=0, tiled=True)
    arrived_gates = lax.all_to_all(packed_gates, "ep", split_axis=0, concat_axis=0, tiled=True)
    full_rows = lax.all_gather(arrived_rows, "tp", axis=2, tiled=True).reshape(slot_count, -1)
    normed = rms_normed(full_rows, norm_gain)
    gate_proj = jnp.einsum("sd,efd->esf", normed, w_gate, preferred_element_type=jnp.float32)
    up_proj = jnp.einsum("sd,efd->esf", normed, w_up, preferred_element_type=jnp.float32)
    hidden = (jax.nn.silu(gate_proj) * up_proj).astype(jnp.bfloat16)
    slot_gates = jnp.transpose(arrived_gates.reshape(slot_count, inner_count))

    def weighted_sum(down_part):
        products = jnp.einsum("esf,efd->esd", hidden, down_part, preferred_element_type=jnp.float32)
        return jnp.sum(slot_gates[:, :, None] * products, axis=0)

    def column_term(first_row, row_count):
        down_part = lax.dynamic_slice_in_dim(w_down, first_row, row_count, 2)
        return jnp.transpose(weighted_sum(down_part))

    own_share = scattered(column_term, feature_share, "tp")
    partial_rows = jnp.transpose(own_share).reshape(ep_size, capacity, feature_share)
    returned = (
        lax.all_to_all(
            partial_rows.astype(jnp.bfloat16), "ep", split_axis=0, concat_axis=0, tiled=True
        )
        .astype(partial_rows.dtype)
        .reshape(slot_count, feature_share)
    )
    mixed_rows = jnp.take(returned, position, axis=0)
    return mixed_rows.astype(jnp.bfloat16)


def solution(mesh):
    square = mesh.shape["ep"] == 4 and mesh.shape["tp"] % 2 == 0
    return jax.shard_map(
        fused if square else per_device,
        mesh=mesh,
        in_specs=(
            P("ep", "tp"),
            P(),
            P("ep", None),
            P("ep", None),
            P("ep", None),
            P("ep", "tp", None),
            P("ep", "tp", None),
            P("ep", "tp", None),
        ),
        out_specs=P("ep", "tp"),
        check_vma=False,
    )
```

```python
import functools

import jax
import jax.numpy as jnp
from jax import lax
from jax.experimental import pallas as pl
from jax.experimental.pallas import tpu as pltpu
from jax.sharding import PartitionSpec as P

epsilon = 1e-06
MESH = pl.DeviceIdType.MESH


def fused_kernel(
    nz,
    tokens_hbm,
    gain_hbm,
    group_hbm,
    inner_hbm,
    route_hbm,
    wg_hbm,
    wu_hbm,
    wd_hbm,
    out,
    tokens,
    gain,
    group_pick,
    inner_pick,
    route_weight,
    wg,
    wu,
    wd,
    rows,
    gates,
    normed,
    hcat,
    to_core,
    from_core,
    part_a,
    part_b,
    in_a1,
    in_b1,
    in_a2,
    in_b2,
    fin,
    in_z,
    w_sem,
    row_send,
    row_recv,
    gate_send,
    gate_recv,
    twin_send,
    twin_recv,
    core_send,
    core_recv,
    xy_send,
    xy_recv,
    z_send,
    z_recv,
):
    ep, tp = lax.axis_index("ep"), lax.axis_index("tp")
    z, core = tp // 2, tp % 2
    twin = (ep, z * 2 + (1 - core))
    peer = [None, (ep ^ 1, tp), (ep ^ 2, tp), (ep ^ 3, tp)]
    tok, share = tokens.shape
    inner = wd_hbm.shape[0]
    width = wd_hbm.shape[1]
    half = share // 2

    def at_z(dz):
        return lax.rem(z + dz, nz)

    loads = [
        pltpu.make_async_copy(src, dst, w_sem.at[i])
        for i, (src, dst) in enumerate(
            (
                (tokens_hbm, tokens),
                (group_hbm, group_pick),
                (inner_hbm, inner_pick),
                (route_hbm, route_weight),
                (gain_hbm, gain),
                (wg_hbm, wg),
                (wu_hbm, wu),
                (wd_hbm, wd),
            )
        )
    ]
    for load in loads:
        load.start()

    barrier = pltpu.get_barrier_semaphore()
    greeted = [twin] + peer[1:] + [(ep, at_z(dz) * 2 + core) for dz in range(1, nz)]
    for device in greeted:
        pl.semaphore_signal(barrier, inc=1, device_id=device, device_id_type=MESH)

    for load in loads[:4]:
        load.wait()
    gate_rows = gates.shape[1]
    row = lax.broadcasted_iota(jnp.int32, (gate_rows, tok), 0)
    relative = (group_pick[...] ^ ep) * inner
    table = jnp.zeros((gate_rows, tok), jnp.float32)
    for k in range(inner_pick.shape[0]):
        key = relative + inner_pick[k : k + 1, :]
        table = table + jnp.where(row == key, route_weight[k : k + 1, :], 0.0)
    gates[0] = jnp.concatenate([table, jnp.zeros((gate_rows, 128 - tok), jnp.float32)], axis=1)
    own = core * nz + z
    rows[0, own] = tokens[...]

    pl.semaphore_wait(barrier, len(greeted))

    sent = []

    def send(src, dst, send_sem, recv_sem, device):
        copy = pltpu.make_async_remote_copy(
            src_ref=src,
            dst_ref=dst,
            send_sem=send_sem,
            recv_sem=recv_sem,
            device_id=device,
            device_id_type=MESH,
        )
        copy.start()
        sent.append(copy)

    def arrived(dst, recv_sem):
        pltpu.make_async_remote_copy(
            src_ref=dst,
            dst_ref=dst,
            send_sem=recv_sem,
            recv_sem=recv_sem,
            device_id=twin,
            device_id_type=MESH,
        ).wait_recv()

    counter = [0]

    def send_row(src, r, t, device):
        i = counter[0]
        counter[0] += 1
        send(src, rows.at[r, t], row_send.at[i], row_recv.at[r, t], device)

    def row_arrived(r, t):
        arrived(rows.at[r, t], row_recv.at[r, t])

    for dz in range(1, nz):
        send_row(tokens, 0, own, (ep, at_z(dz) * 2 + core))
    send_row(tokens, 1, own, peer[1])
    send_row(tokens, 2, own, peer[2])

    def share_rows(r):
        mine = rows.at[r, pl.ds(core * nz, nz)]
        send(mine, mine, twin_send.at[r], twin_recv.at[r], twin)

    for r in range(1, 4):
        send(gates.at[0], gates.at[r], gate_send.at[r], gate_recv.at[r], peer[r])
    order = sorted(range(nz), key=lambda dz: min(dz, nz - dz))
    for dz in order[1:]:
        t = core * nz + at_z(dz)
        row_arrived(0, t)
        send_row(rows.at[0, t], 1, t, peer[1])
        send_row(rows.at[0, t], 2, t, peer[2])

    columns = []

    def norm(r):
        if r > 0:
            arrived(gates.at[r], gate_recv.at[r])
        arrived(rows.at[r, pl.ds((1 - core) * nz, nz)], twin_recv.at[r])
        total = jnp.zeros((tok, 1), jnp.float32)
        for t in range(2 * nz):
            piece = rows[r, (t % 2) * nz + t // 2].astype(jnp.float32)
            total = total + jnp.sum(piece * piece, axis=1, keepdims=True)
        scaled = lax.rsqrt(total / (2 * nz * share) + epsilon)
        for t in range(2 * nz):
            piece = rows[r, (t % 2) * nz + t // 2].astype(jnp.float32)
            span = slice(t * share, (t + 1) * share)
            normed[r * tok : (r + 1) * tok, span] = (piece * scaled * gain[:, span]).astype(jnp.bfloat16)
        turned = jnp.transpose(gates[r])[:tok]
        columns.append([turned[:, r * inner + e : r * inner + e + 1] for e in range(inner)])

    share_rows(0)
    loads[4].wait()
    norm(0)
    for i, dz in enumerate(order):
        t = core * nz + at_z(dz)
        row_arrived(1, t)
        if i % 2 == 0:
            send_row(rows.at[1, t], 3, t, peer[2])
        row_arrived(2, t)
        if i % 2 == 1:
            send_row(rows.at[2, t], 3, t, peer[1])
    share_rows(1)
    share_rows(2)
    norm(1)
    norm(2)
    for dz in order:
        t = core * nz + at_z(dz)
        row_arrived(3, t)
    share_rows(3)
    norm(3)

    loads[5].wait()
    loads[6].wait()
    count = 4 * tok
    contract = (((1,), (1,)), ((), ()))
    for e in range(0, inner, 2):
        pair = wg[e : e + 2].reshape(2 * width, -1)
        gate_proj = lax.dot_general(normed[...], pair, contract, preferred_element_type=jnp.float32)
        pair = wu[e : e + 2].reshape(2 * width, -1)
        up_proj = lax.dot_general(normed[...], pair, contract, preferred_element_type=jnp.float32)
        hidden = gate_proj / (1.0 + jnp.exp(-gate_proj)) * up_proj
        hidden = hidden.astype(jnp.bfloat16).astype(jnp.float32)
        for j in range(2):
            weight = jnp.concatenate([columns[r][e + j] for r in range(4)], axis=0)
            weighted = hidden[:, j * width : (j + 1) * width] * weight
            high = weighted.astype(jnp.bfloat16)
            low = (weighted - high.astype(jnp.float32)).astype(jnp.bfloat16)
            span = slice((e + j) * width, (e + j + 1) * width)
            hcat[:count, span] = high
            hcat[count:, span] = low

    loads[7].wait()

    def down(t):
        cols = pl.ds(pl.multiple_of(t * share, share), share)
        both = jnp.dot(
            hcat[...],
            wd[:, :, cols].reshape(inner * width, share),
            preferred_element_type=jnp.float32,
        )
        return both[:count] + both[count:]

    offsets = sorted(range(1, nz), key=lambda dz: -min(dz, nz - dz)) + [0]

    def first(k):
        dz = offsets[k]
        to_core[k] = down(at_z(dz) * 2 + (1 - core))
        send(to_core.at[k], from_core.at[k], core_send.at[k], core_recv.at[k], twin)
        mine = down(at_z(dz) * 2 + core)
        arrived(from_core.at[k], core_recv.at[k])
        for slot in range(4):
            ra = (0, 2, 1, 3)[slot]
            part_a[k, slot] = (
                mine[ra * tok : (ra + 1) * tok, :half] + from_core[k, ra * tok : (ra + 1) * tok, :half]
            )
            part_b[k, slot] = (
                mine[slot * tok : (slot + 1) * tok, half:] + from_core[k, slot * tok : (slot + 1) * tok, half:]
            )
        send(part_a.at[k, pl.ds(2, 2)], in_a1.at[k], xy_send.at[k, 0], xy_recv.at[k, 0], peer[1])
        send(part_b.at[k, pl.ds(2, 2)], in_b1.at[k], xy_send.at[k, 1], xy_recv.at[k, 1], peer[2])

    def second(k):
        arrived(in_a1.at[k], xy_recv.at[k, 0])
        part_a[k, 1] += in_a1[k, 1]
        send(part_a.at[k, 1], in_a2.at[k], xy_send.at[k, 2], xy_recv.at[k, 2], peer[2])
        arrived(in_b1.at[k], xy_recv.at[k, 1])
        part_b[k, 1] += in_b1[k, 1]
        send(part_b.at[k, 1], in_b2.at[k], xy_send.at[k, 3], xy_recv.at[k, 3], peer[1])

    def last(k):
        arrived(in_a2.at[k], xy_recv.at[k, 2])
        fin[k, :, :half] = part_a[k, 0] + in_a1[k, 0] + in_a2[k]
        arrived(in_b2.at[k], xy_recv.at[k, 3])
        fin[k, :, half:] = part_b[k, 0] + in_b1[k, 0] + in_b2[k]
        if offsets[k] != 0:
            device = (ep, at_z(offsets[k]) * 2 + core)
            send(fin.at[k], in_z.at[k], z_send.at[k], z_recv.at[k], device)

    for k in range(nz + 3):
        if k < nz:
            first(k)
        if 0 <= k - 1 < nz:
            second(k - 1)
        if 0 <= k - 2 < nz:
            last(k - 2)
    total = fin[nz - 1]
    for k in range(nz - 1):
        arrived(in_z.at[k], z_recv.at[k])
        total = total + in_z[k]
    out[...] = total.astype(out.dtype)
    for copy in sent:
        copy.wait_send()


def fused(tokens, norm_gain, group_pick, inner_pick, route_weight, w_gate, w_up, w_down):
    tp_size = lax.axis_size("tp")
    nz = tp_size // 2
    tok, share = tokens.shape
    inner, width, features = w_gate.shape
    half = share // 2
    top = inner_pick.shape[1]
    count = 4 * tok
    gate_rows = -(-4 * inner // 8) * 8
    f32, bf16 = jnp.float32, jnp.bfloat16
    vmem = pl.BlockSpec(memory_space=pltpu.VMEM)
    hbm = pl.BlockSpec(memory_space=pl.ANY)
    dma = pltpu.SemaphoreType.DMA
    sends = (nz - 1) + 2 + 2 * (nz - 1) + nz
    return pl.pallas_call(
        functools.partial(fused_kernel, nz),
        out_shape=jax.ShapeDtypeStruct((tok, share), bf16),
        in_specs=[hbm] * 8,
        out_specs=vmem,
        scratch_shapes=[
            pltpu.VMEM((tok, share), bf16),
            pltpu.VMEM((1, features), f32),
            pltpu.VMEM((1, tok), jnp.int32),
            pltpu.VMEM((top, tok), jnp.int32),
            pltpu.VMEM((top, tok), f32),
            pltpu.VMEM((inner, width, features), bf16),
            pltpu.VMEM((inner, width, features), bf16),
            pltpu.VMEM((inner, width, features), bf16),
            pltpu.VMEM((4, tp_size, tok, share), bf16),
            pltpu.VMEM((4, gate_rows, 128), f32),
            pltpu.VMEM((count, features), bf16),
            pltpu.VMEM((2 * count, inner * width), bf16),
            pltpu.VMEM((nz, count, share), f32),
            pltpu.VMEM((nz, count, share), f32),
            pltpu.VMEM((nz, 4, tok, half), f32),
            pltpu.VMEM((nz, 4, tok, half), f32),
            pltpu.VMEM((nz, 2, tok, half), f32),
            pltpu.VMEM((nz, 2, tok, half), f32),
            pltpu.VMEM((nz, tok, half), f32),
            pltpu.VMEM((nz, tok, half), f32),
            pltpu.VMEM((nz, tok, share), f32),
            pltpu.VMEM((nz, tok, share), f32),
            dma((8,)),
            dma((sends,)),
            dma((4, tp_size)),
            dma((4,)),
            dma((4,)),
            dma((4,)),
            dma((4,)),
            dma((nz,)),
            dma((nz,)),
            dma((nz, 4)),
            dma((nz, 4)),
            dma((nz,)),
            dma((nz,)),
        ],
        compiler_params=pltpu.CompilerParams(
            collective_id=0, has_side_effects=True, vmem_limit_bytes=67043328
        ),
    )(
        tokens,
        norm_gain.reshape(1, -1),
        group_pick.T,
        inner_pick.T,
        route_weight.T,
        w_gate,
        w_up,
        w_down,
    )


def scattered(portion, rows, axis):
    count = rows * lax.axis_size(axis)
    return lax.psum_scatter(portion(jnp.int32(0), count), axis, scatter_dimension=0, tiled=True)


def rms_normed(rows, norm_gain):
    widened = rows.astype(jnp.float32)
    scaled = lax.rsqrt(jnp.mean(widened * widened, axis=-1, keepdims=True) + epsilon)
    return (widened * scaled * norm_gain).astype(jnp.bfloat16)


def per_device(tokens, norm_gain, group_pick, inner_pick, route_weight, w_gate, w_up, w_down):
    ep_size = lax.axis_size("ep")
    tok_rows = tokens.shape[0]
    feature_share = tokens.shape[1]
    inner_count = w_gate.shape[0]
    capacity = min(tok_rows, 4 * tok_rows // ep_size + 2)
    slot_count = ep_size * capacity
    groups = group_pick[:, 0]
    member = (groups[:, None] == jnp.arange(ep_size, dtype=jnp.int32)[None, :]).astype(jnp.int32)
    earlier = jnp.sum((jnp.cumsum(member, axis=0) - member) * member, axis=1)
    position = (groups * capacity + earlier).astype(jnp.int32)
    placing = position[None, :] == jnp.arange(slot_count, dtype=jnp.int32)[:, None]
    local_gates = jnp.sum(
        jax.nn.one_hot(inner_pick, inner_count, dtype=jnp.float32) * route_weight[:, :, None],
        axis=1,
    )
    packed_rows = jnp.dot(
        placing.astype(jnp.bfloat16), tokens, preferred_element_type=jnp.float32
    ).astype(jnp.bfloat16)
    packed_gates = jnp.dot(
        placing.astype(jnp.float32), local_gates, precision=lax.Precision.HIGHEST
    )
    packed_rows = packed_rows.reshape(ep_size, capacity, feature_share)
    packed_gates = packed_gates.reshape(ep_size, capacity, inner_count)
    arrived_rows = lax.all_to_all(packed_rows, "ep", split_axis=0, concat_axis=0, tiled=True)
    arrived_gates = lax.all_to_all(packed_gates, "ep", split_axis=0, concat_axis=0, tiled=True)
    full_rows = lax.all_gather(arrived_rows, "tp", axis=2, tiled=True).reshape(slot_count, -1)
    normed = rms_normed(full_rows, norm_gain)
    gate_proj = jnp.einsum("sd,efd->esf", normed, w_gate, preferred_element_type=jnp.float32)
    up_proj = jnp.einsum("sd,efd->esf", normed, w_up, preferred_element_type=jnp.float32)
    hidden = (jax.nn.silu(gate_proj) * up_proj).astype(jnp.bfloat16)
    slot_gates = jnp.transpose(arrived_gates.reshape(slot_count, inner_count))

    def weighted_sum(down_part):
        products = jnp.einsum("esf,efd->esd", hidden, down_part, preferred_element_type=jnp.float32)
        return jnp.sum(slot_gates[:, :, None] * products, axis=0)

    def column_term(first_row, row_count):
        down_part = lax.dynamic_slice_in_dim(w_down, first_row, row_count, 2)
        return jnp.transpose(weighted_sum(down_part))

    own_share = scattered(column_term, feature_share, "tp")
    partial_rows = jnp.transpose(own_share).reshape(ep_size, capacity, feature_share)
    returned = (
        lax.all_to_all(
            partial_rows.astype(jnp.bfloat16), "ep", split_axis=0, concat_axis=0, tiled=True
        )
        .astype(partial_rows.dtype)
        .reshape(slot_count, feature_share)
    )
    mixed_rows = jnp.take(returned, position, axis=0)
    return mixed_rows.astype(jnp.bfloat16)


def solution(mesh):
    square = mesh.shape["ep"] == 4 and mesh.shape["tp"] % 2 == 0
    return jax.shard_map(
        fused if square else per_device,
        mesh=mesh,
        in_specs=(
            P("ep", "tp"),
            P(),
            P("ep", None),
            P("ep", None),
            P("ep", None),
            P("ep", "tp", None),
            P("ep", "tp", None),
            P("ep", "tp", None),
        ),
        out_specs=P("ep", "tp"),
        check_vma=False,
    )
```
